256 devices in a mesh: ep: 16 (over y, x), tp: 16 (over z, core).
Axes of the slice: x: 4, y: 4, z: 8, core: 2. Of those that a mesh axis runs over, the one named last changes fastest.
Arguments:
- resid: bfloat16 [2048, 2048], P('ep'), may hold values from -6 to 6
- norm1_gain: float32 [2048], replicated, may hold values from 0.1 to 1.9
- w_query: bfloat16 [2048, 2048], P('ep', 'tp'), may hold values from -0.125 to 0.125
- w_key: bfloat16 [2048, 2048], P('ep', 'tp'), may hold values from -0.125 to 0.125
- w_value: bfloat16 [2048, 2048], P('ep', 'tp'), may hold values from -0.125 to 0.125
- w_outgate: bfloat16 [2048, 2048], P('ep', 'tp'), may hold values from -0.125 to 0.125
- w_igate: bfloat16 [2048, 32], replicated, may hold values from -0.125 to 0.125
- w_fgate: bfloat16 [2048, 32], replicated, may hold values from -0.125 to 0.125
- forget_bias: float32 [32], replicated, may hold values from 0 to 4
- head_gain: float32 [2048], P('tp'), may hold values from 0.1 to 1.9
- w_out: bfloat16 [2048, 2048], P('tp'), may hold values from -0.125 to 0.125
- state_matrix: float32 [2048, 32, 64, 64], P('ep', 'tp'), may hold values from -4 to 4
- state_norm: float32 [2048, 32, 64], P('ep', 'tp'), may hold values from -8 to 8
- state_max: float32 [2048, 32], P('ep', 'tp'), may hold values from -1 to 2
- norm2_gain: float32 [2048], replicated, may hold values from 0.1 to 1.9
- group_router: bfloat16 [2048, 4], replicated, may hold values from -0.125 to 0.125
- expert_router: bfloat16 [2048, 32], replicated, may hold values from -0.125 to 0.125
- expert_ids: int32 [2048, 2], P('ep'), may hold values from 0 to 31, all different within a row; in each aligned block of 128 rows (0 to 127, 128 to 255, ...) at most 12 rows name the same one
- exp_gate: bfloat16 [32, 2048, 1024], P('ep', None, 'tp'), may hold values from -0.125 to 0.125
- exp_up: bfloat16 [32, 2048, 1024], P('ep', None, 'tp'), may hold values from -0.125 to 0.125
- exp_down: bfloat16 [32, 1024, 2048], P('ep', 'tp'), may hold values from -0.1875 to 0.1875
Outputs:
- mixed: bfloat16 [2048, 2048], P('ep', 'tp')
- new_matrix: float32 [2048, 32, 64, 64], P('ep', 'tp')
- new_normer: float32 [2048, 32, 64], P('ep', 'tp')
- new_max: float32 [2048, 32], P('ep', 'tp')
The draws below stay inside these ranges and needn't reach their ends.
Inputs may be any that keep to these rules, and one draw needn't show every extreme that they name: `expert_ids`: A token's 2 experts differ. Among the 128 tokens of one index of ep (aligned blocks of rows) no expert is named more than 12 times, and in some block one expert is named exactly 12 times.
All inputs are finite; a program needn't handle non-finite values.
Results may differ from the reference program's by a relative error of at most 0.014.
Values may be sent and summed in bfloat16 or wider, within the bound.
A program may use at most 128 MiB of HBM per device.

```python
import math
import jax
import jax.numpy as jnp
import numpy as np
from jax import lax

D = 2048
HEADS = 32
DK = 64
FF = 1024
N_GROUPS = 4
TOPK = 2
SEQ_GRP = 128
TOKENS = 2048
EXPERTS = 32
EXP_GROUP = 8
CAP = 12
N_EP = 16


def steps_of(rng, shape, split, low, largest):
    loudness = 1.0
    for axis_at, shards_of in split:
        draws = jax.random.uniform(jax.random.fold_in(jax.random.fold_in(rng, 6), axis_at), (shards_of,), jnp.float32, low / len(split), largest / len(split))
        loudness = loudness * jnp.repeat(jnp.exp(draws), shape[axis_at] // shards_of).reshape((-1,) + (1,) * (len(shape) - 1 - axis_at))
    return loudness


def routed_block(own_key, own, number, rows, amount, top, most, slope):
    order = jax.random.permutation(own_key, amount)
    packed, usual = shares(amount, rows * top, most, slope, True), shares(amount, rows * top, most, slope, False)
    places = jnp.arange(amount)

    def named(tallies, turn):
        used = int((tallies > 0).sum())
        fixed = max(1, used // 4)
        shifted = fixed + (places - fixed + turn * (used - fixed)) % max(1, amount - fixed)
        return jnp.zeros((amount,), jnp.int32).at[order[jnp.where(places < fixed, places, shifted)]].set(jnp.asarray(tallies, jnp.int32))

    tallies = jnp.where(number % 4 == 0, named(packed, number // 4), named(usual, number - number // 4 - 1))
    mixed = jax.random.permutation(jax.random.fold_in(own, 3), amount)
    giver, receiver = mixed[0:amount // 2 * 2:2], mixed[1:amount // 2 * 2:2]
    slack = jnp.minimum(tallies[giver] - 1, most - tallies[receiver]) // 2
    slack = jnp.where((giver == order[0]) | (receiver == order[0]) | (tallies[receiver] == 0), 0, jnp.maximum(slack, 0))
    shifted = jax.random.randint(jax.random.fold_in(own, 4), (amount // 2,), 0, 1 << 20) % (slack + 1)
    tallies = tallies.at[giver].add(-shifted).at[receiver].add(shifted)
    labels = jnp.searchsorted(jnp.cumsum(tallies), jnp.arange(rows * top), side="right").astype(jnp.int32)
    grid = labels.reshape(top, rows).T
    grid = grid[jax.random.permutation(jax.random.fold_in(own, 1), rows)]
    turn = jax.random.randint(jax.random.fold_in(own, 2), (rows, 1), 0, top)
    return jnp.take_along_axis(grid, (jnp.arange(top)[None, :] + turn) % top, axis=1)


def shares(amount, total, bound, slope, full):
    loads = [(1 << 20) // math.isqrt(standing ** slope) + 1 for standing in range(1, amount + 1)]
    largest = bound if full else min(bound, max(-(-total // amount), total * loads[0] // sum(loads)))
    least = 1 if total - largest >= amount - 1 else 0
    holding, surplus = [largest] + [least] * (amount - 1), total - largest - least * (amount - 1)
    while surplus > 0:
        candidates = [i for i in range(1, amount) if holding[i] < largest] or [i for i in range(1, amount) if holding[i] < bound]
        whole, left = sum([loads[i] for i in candidates]), surplus
        for i in candidates:
            more = min(bound - holding[i], max(1, left * loads[i] // whole), surplus)
            holding[i] = holding[i] + more
            surplus = surplus - more
    return np.array(holding)


def normal_values(key, shape, spread, bound, cuts=(), kind=jnp.bfloat16):
    factor_of = steps_of(key, shape, cuts, -0.22, 0.18) if cuts else 1.0
    result = jax.random.normal(key, shape, jnp.float32) * spread * factor_of
    return jnp.minimum(jnp.maximum(result, -bound), bound).astype(kind)


def setup_inputs(seed: int = 0) -> dict:
    keys = jax.random.split(jax.random.key(seed), 22)
    resid = normal_values(keys[0], (TOKENS, D), 1.0, 6.0, ((0, 16),))
    norm1_gain = jnp.clip(1.0 + 0.18 * jax.random.normal(keys[1], (D,), jnp.float32), 0.1, 1.9)
    w_query = normal_values(keys[2], (D, HEADS * DK), D ** -0.5, 0.125, ((0, 16), (1, 16)))
    w_key = normal_values(keys[3], (D, HEADS * DK), D ** -0.5, 0.125, ((0, 16), (1, 16)))
    w_value = normal_values(keys[4], (D, HEADS * DK), D ** -0.5, 0.125, ((0, 16), (1, 16)))
    w_outgate = normal_values(keys[5], (D, HEADS * DK), D ** -0.5, 0.125, ((0, 16), (1, 16)))
    w_igate = normal_values(keys[6], (D, HEADS), D ** -0.5, 0.125)
    w_fgate = normal_values(keys[7], (D, HEADS), D ** -0.5, 0.125)
    forget_bias = jnp.clip(jax.random.uniform(keys[8], (HEADS,), jnp.float32, 0.0, 4.0), 0.0, 4.0)
    head_gain = jnp.clip(1.0 + 0.18 * jax.random.normal(keys[9], (HEADS * DK,), jnp.float32), 0.1, 1.9)
    w_out = normal_values(keys[10], (HEADS * DK, D), (HEADS * DK) ** -0.5, 0.125, ((0, 16),))
    state_matrix = normal_values(keys[11], (TOKENS, HEADS, DK, DK), 0.5, 4.0, ((0, 16), (1, 16)), jnp.float32)
    state_norm = normal_values(keys[12], (TOKENS, HEADS, DK), 2.0, 8.0, ((0, 16), (1, 16)), jnp.float32)
    state_max = jnp.clip(-1.0 + 3.0 * jax.random.uniform(keys[13], (TOKENS, HEADS), jnp.float32) ** steps_of(keys[13], (TOKENS, HEADS), ((0, 16), (1, 16)), -0.2, 0.2), -1.0, 2.0)
    norm2_gain = jnp.clip(1.0 + 0.18 * jax.random.normal(keys[14], (D,), jnp.float32), 0.1, 1.9)
    group_router = normal_values(keys[15], (D, N_GROUPS), D ** -0.5, 0.125)
    expert_router = normal_values(keys[16], (D, EXPERTS), D ** -0.5, 0.125)
    expert_ids_keys = jax.random.split(jax.random.fold_in(keys[17], 1), TOKENS // SEQ_GRP)
    expert_ids_turns = jax.random.permutation(jax.random.fold_in(keys[17], 3), TOKENS // SEQ_GRP)
    expert_ids = jax.vmap(lambda own, number: routed_block(jax.random.fold_in(keys[17], 2), own, number, SEQ_GRP, EXPERTS, TOPK, CAP, 2))(expert_ids_keys, expert_ids_turns).reshape((TOKENS, TOPK))
    exp_gate = normal_values(keys[18], (EXPERTS, D, FF), D ** -0.5, 0.125, ((0, 16), (2, 16)))
    exp_up = normal_values(keys[19], (EXPERTS, D, FF), D ** -0.5, 0.125, ((0, 16), (2, 16)))
    exp_down = normal_values(keys[20], (EXPERTS, FF, D), FF ** -0.5, 0.1875, ((0, 16), (1, 16)))
    return {"resid": resid, "norm1_gain": norm1_gain, "w_query": w_query, "w_key": w_key, "w_value": w_value, "w_outgate": w_outgate, "w_igate": w_igate, "w_fgate": w_fgate, "forget_bias": forget_bias, "head_gain": head_gain, "w_out": w_out, "state_matrix": state_matrix, "state_norm": state_norm, "state_max": state_max, "norm2_gain": norm2_gain, "group_router": group_router, "expert_router": expert_router, "expert_ids": expert_ids, "exp_gate": exp_gate, "exp_up": exp_up, "exp_down": exp_down}


EPSILON = 1e-06

def rms_scale(values, gain):
    widened = values.astype(jnp.float32)
    factor = lax.rsqrt(lax.optimization_barrier(jnp.mean(widened * widened, axis=-1, keepdims=True)) + EPSILON)
    return widened * factor * gain.astype(jnp.float32)

def memory_cell(scaled, key_rows, value_rows, in_gate, log_forget, matrix, normer, running):
    stable = jnp.maximum(log_forget + running, in_gate)
    fresh = jnp.exp(in_gate - stable)
    carried = jnp.exp(log_forget + running - stable)
    readout = jnp.einsum('bhd,bhde->bhe', scaled, matrix, precision=lax.Precision.HIGHEST)
    score = lax.optimization_barrier(jnp.sum(scaled * key_rows, axis=-1)) * fresh
    numer = carried[..., None] * readout + score[..., None] * value_rows
    denom = carried * lax.optimization_barrier(jnp.sum(scaled * normer, axis=-1)) + score
    cell_out = numer / jnp.maximum(jnp.abs(denom), 1.0)[..., None]
    new_matrix = carried[..., None, None] * matrix + fresh[..., None, None] * key_rows[..., :, None] * value_rows[..., None, :]
    new_normer = carried[..., None] * normer + fresh[..., None] * key_rows
    return (cell_out, new_matrix, new_normer, stable)

def reference(resid, norm1_gain, w_query, w_key, w_value, w_outgate, w_igate, w_fgate, forget_bias, head_gain, w_out, state_matrix, state_norm, state_max, norm2_gain, group_router, expert_router, expert_ids, exp_gate, exp_up, exp_down):
    rows = resid.shape[0]
    heads = state_matrix.shape[1]
    size = state_matrix.shape[2]
    normed = rms_scale(resid, norm1_gain).astype(jnp.bfloat16)

    def project(weight):
        product = jnp.dot(normed, weight, preferred_element_type=jnp.float32)
        stored = lax.optimization_barrier(product.astype(jnp.bfloat16))
        return stored.astype(jnp.float32).reshape(rows, heads, size)
    scaled = project(w_query) * size ** (-0.5)
    key_rows = project(w_key)
    value_rows = project(w_value)
    outgate = project(w_outgate)
    in_gate = jnp.dot(normed, w_igate, preferred_element_type=jnp.float32)
    log_forget = jax.nn.log_sigmoid(jnp.dot(normed, w_fgate, preferred_element_type=jnp.float32) + forget_bias)
    cell_out, new_matrix, new_normer, new_max = memory_cell(scaled, key_rows, value_rows, in_gate, log_forget, state_matrix, state_norm, state_max)
    headed = cell_out * lax.rsqrt(lax.optimization_barrier(jnp.mean(cell_out * cell_out, axis=-1, keepdims=True)) + EPSILON)
    headed = headed * head_gain.reshape(heads, size) * jax.nn.sigmoid(outgate)
    head_out = headed.astype(jnp.bfloat16).reshape(rows, heads * size)
    after_mix = (resid.astype(jnp.float32) + jnp.dot(head_out, w_out, preferred_element_type=jnp.float32)).astype(jnp.bfloat16)
    normed2 = rms_scale(after_mix, norm2_gain).astype(jnp.bfloat16)
    group_exp = jnp.exp(jnp.dot(normed2, group_router, preferred_element_type=jnp.float32))
    group_prob = group_exp / lax.optimization_barrier(jnp.sum(group_exp, axis=1, keepdims=True))
    expert_logits = jnp.dot(normed2, expert_router, preferred_element_type=jnp.float32)
    chosen_exp = jnp.exp(jnp.take_along_axis(expert_logits, expert_ids, axis=1))
    share = chosen_exp / lax.optimization_barrier(jnp.sum(chosen_exp, axis=1, keepdims=True))
    group_weight = jnp.take_along_axis(group_prob, expert_ids // EXP_GROUP, axis=1)
    route_weight = group_weight * share
    limit = CAP * N_EP

    def one_expert(total, inputs):
        expert_index, gate_w, up_w, down_w = inputs
        picked = expert_ids == expert_index
        coeff = lax.optimization_barrier(jnp.sum(jnp.where(picked, route_weight, 0.0), axis=1))
        member = jnp.any(picked, axis=1)
        count = jnp.sum(member.astype(jnp.int32))
        places = jnp.nonzero(member, size=limit, fill_value=0)[0].astype(jnp.int32)
        valid = (jnp.arange(limit, dtype=jnp.int32) < count).astype(jnp.float32)
        taken = normed2[places]
        gate_part = jnp.dot(taken, gate_w, preferred_element_type=jnp.float32)
        up_part = jnp.dot(taken, up_w, preferred_element_type=jnp.float32)
        units = (jax.nn.silu(gate_part) * up_part).astype(jnp.bfloat16)
        expert_out = jnp.dot(units, down_w, preferred_element_type=jnp.float32)
        total = total.at[places].add(expert_out * (coeff[places] * valid)[:, None])
        return (total, None)
    start_total = jnp.zeros((rows, resid.shape[1]), jnp.float32)
    moe, _ = lax.scan(one_expert, start_total, (jnp.arange(EXPERTS, dtype=jnp.int32), exp_gate, exp_up, exp_down))
    mixed = (after_mix.astype(jnp.float32) + moe).astype(jnp.bfloat16)
    return (mixed, new_matrix, new_normer, new_max)
```

```python
import functools

import jax
import jax.numpy as jnp
from jax import lax
from jax.experimental import pallas as pl
from jax.experimental.pallas import tpu as pltpu
from jax.sharding import PartitionSpec as P

EPS = 1e-06
F32 = jnp.float32
BF16 = jnp.bfloat16
MESH = pl.DeviceIdType.MESH
SX, SY, SZ = 4, 4, 8
NEP = SX * SY
CAP = 12
ROWS = 2 * CAP
SLOTS = NEP * ROWS
HALF = SLOTS // 2
NREM = 192
NLOC = 24


def mm(a, b):
    return lax.dot_general(a, b, (((1,), (0,)), ((), ())), preferred_element_type=F32)


def mmt(a, b):
    return lax.dot_general(a, b, (((1,), (1,)), ((), ())), preferred_element_type=F32)


def by12(v):
    return (v * 43691) >> 19


def kernel(
    resid_hbm, g1, wq_hbm, wk_hbm, wv_hbm, wo_hbm, igt, fgt, bias, hgain, wout_hbm,
    st_hbm, nrm, smax, g2, grt, ert, ids, gate_hbm, up_hbm, down_hbm,
    mixed, newmat_hbm, newnrm, newmax,
    resid_v, normed_v, wga, wgb, gates_v, st, qt, fkt, hg, wob, att, attr,
    disp, dispt, perm, permt, meta, metar, metap, dsp, rx, xg,
    gate_v, up_v, down_v, wall, wst, dn, dst, sb, sr, wgt, pbuf, sbuf, rbuf, sx, ret, after_v,
    ssem, rsem, lsem,
):
    e = lax.axis_index("ep")
    t = lax.axis_index("tp")
    y, x = e // SX, lax.rem(e, SX)
    z, c = t // 2, lax.rem(t, 2)
    count = [0, 0]
    sent = []

    def new_id():
        count[0] += 1
        return count[0] - 1

    def rdma(k, src, dst, dev):
        copy = pltpu.make_async_remote_copy(
            src_ref=src, dst_ref=dst, send_sem=ssem.at[k], recv_sem=rsem.at[k],
            device_id=dev, device_id_type=MESH,
        )
        copy.start()
        sent.append(copy)

    def arrived(k, region, dev):
        pltpu.make_async_remote_copy(
            src_ref=region, dst_ref=region, send_sem=ssem.at[k], recv_sem=rsem.at[k],
            device_id=dev, device_id_type=MESH,
        ).wait_recv()

    def local(src, dst):
        k = count[1]
        count[1] += 1
        copy = pltpu.make_async_copy(src, dst, lsem.at[k])
        copy.start()
        return copy

    def peer_ep(k):
        return lax.rem(e + k, NEP)

    def at_xy(dx, dy):
        return lax.rem(y + dy + SY, SY) * SX + lax.rem(x + dx + SX, SX)

    def zoff(k):
        return lax.rem(z + k + SZ, SZ)

    partner = (e, 2 * z + 1 - c)

    own = pl.ds(pl.multiple_of(e * 128, 128), 128)
    l_wa = [local(wq_hbm, wga.at[own, pl.ds(0, 128)]), local(wk_hbm, wga.at[own, pl.ds(128, 128)])]
    l_wb = [local(wv_hbm, wgb.at[own, pl.ds(0, 128)]), local(wo_hbm, wgb.at[own, pl.ds(128, 128)])]
    l_resid = local(resid_hbm, resid_v)

    barrier = pltpu.get_barrier_semaphore()
    peers = [(peer_ep(k), t) for k in range(1, NEP)]
    peers += [(e, 2 * zoff(k) + c) for k in range(1, SZ)] + [partner]
    for p in peers:
        pl.semaphore_signal(barrier, inc=1, device_id=p, device_id_type=MESH)

    zown = pl.ds(pl.multiple_of(z * 128, 128), 128)
    l_wob = local(wout_hbm.at[:, pl.ds(pl.multiple_of(z * 256, 256), 256)], wob.at[zown, :])
    l_state = local(st_hbm, st)
    l_gate = local(gate_hbm, gate_v)
    l_up = local(up_hbm, up_v)
    l_down = local(down_hbm, down_v)

    pl.semaphore_wait(barrier, len(peers))
    for cp in l_wa + l_wb:
        cp.wait()

    halves = []
    for wg, first in ((wga, "x"), (wgb, "y")):
        def dev(a1, a2, first=first):
            return at_xy(a1, a2) if first == "x" else at_xy(a2, a1)

        def blk(a1, a2, part, wg=wg, dev=dev):
            base = dev(a1, a2) * 128
            if part is None:
                return wg.at[pl.ds(pl.multiple_of(base, 128), 128), :]
            return wg.at[pl.ds(pl.multiple_of(base + part * 64, 64), 64), :]

        halves.append((dev, blk))

    ids1 = [{k: new_id() for k in ("p", "m", "fp", "fm")} for _ in halves]
    ids2 = [{(b, k): new_id() for b in range(4) for k in ("p", "m", "fp", "fm")} for _ in halves]
    offs = (0, -1, 1, 2)

    def stage2_start(h, b):
        dev, blk = halves[h]
        rdma(ids2[h][b, "p"], blk(offs[b], 0, None), blk(offs[b], 0, None), (dev(0, 1), t))
        rdma(ids2[h][b, "m"], blk(offs[b], 0, None), blk(offs[b], 0, None), (dev(0, -1), t))

    for h, (dev, blk) in enumerate(halves):
        rdma(ids1[h]["p"], blk(0, 0, None), blk(0, 0, None), (dev(1, 0), t))
        rdma(ids1[h]["m"], blk(0, 0, None), blk(0, 0, None), (dev(-1, 0), t))
    for h in range(2):
        stage2_start(h, 0)

    wout_ids = {}
    for k in range(1, SZ):
        wout_ids[k] = new_id()
        zk = zoff(k)
        rdma(
            wout_ids[k], wout_hbm.at[:, pl.ds(pl.multiple_of(zk * 256, 256), 256)],
            wob.at[zown, :], (e, 2 * zk + c),
        )

    l_resid.wait()
    wide = resid_v[...].astype(F32)
    factor = lax.rsqrt(jnp.mean(wide * wide, axis=1, keepdims=True) + EPS)
    normed_v[...] = (wide * factor * g1[...]).astype(BF16)

    for h, (dev, blk) in enumerate(halves):
        arrived(ids1[h]["p"], blk(-1, 0, None), (dev(-1, 0), t))
        rdma(ids1[h]["fp"], blk(-1, 0, 0), blk(-1, 0, 0), (dev(1, 0), t))
        arrived(ids1[h]["m"], blk(1, 0, None), (dev(1, 0), t))
        rdma(ids1[h]["fm"], blk(1, 0, 1), blk(1, 0, 1), (dev(-1, 0), t))
    for b in (1, 2):
        for h in range(2):
            stage2_start(h, b)

    gates_v[0:32, :] = mmt(igt[...], normed_v[...])
    gates_v[32:64, :] = mmt(fgt[...], normed_v[...])

    def stage2_forward(h, b):
        dev, blk = halves[h]
        arrived(ids2[h][b, "p"], blk(offs[b], -1, None), (dev(0, -1), t))
        rdma(ids2[h][b, "fp"], blk(offs[b], -1, 0), blk(offs[b], -1, 0), (dev(0, 1), t))
        arrived(ids2[h][b, "m"], blk(offs[b], 1, None), (dev(0, 1), t))
        rdma(ids2[h][b, "fm"], blk(offs[b], 1, 1), blk(offs[b], 1, 1), (dev(0, -1), t))

    for h in range(2):
        stage2_forward(h, 0)
    for h, (dev, blk) in enumerate(halves):
        arrived(ids1[h]["fp"], blk(2, 0, 0), (dev(-1, 0), t))
        arrived(ids1[h]["fm"], blk(2, 0, 1), (dev(1, 0), t))
        stage2_start(h, 3)

    srow = lax.broadcasted_iota(jnp.int32, (SLOTS, 128), 0)
    s_exp = by12(srow)
    s_cap = srow - s_exp * CAP
    assigned = jnp.where((ids[0:1, :] == s_exp) | (ids[1:2, :] == s_exp), 1.0, 0.0)
    earlier = jnp.where(
        lax.broadcasted_iota(jnp.int32, (128, 128), 0) < lax.broadcasted_iota(jnp.int32, (128, 128), 1),
        1.0, 0.0,
    ).astype(BF16)
    rank = mm(assigned.astype(BF16), earlier)
    hot = jnp.where(jnp.abs(rank - s_cap.astype(F32)) < 0.5, assigned, 0.0)
    disp[...] = hot.astype(BF16)
    dispt[...] = hot.T.astype(BF16)
    erow = lax.broadcasted_iota(jnp.int32, (128, 128), 0)
    chosen = jnp.where((ids[0:1, :] == erow) | (ids[1:2, :] == erow), 1.0, 0.0).T.astype(BF16)
    meta[...] = mm(disp[...], chosen)

    for h in range(2):
        for b in (1, 2):
            stage2_forward(h, b)

    def slot_of(r):
        i = jnp.where(r >= HALF, 1, 0)
        q = r - i * HALF
        s = by12(q)
        return s * ROWS + i * CAP + (q - s * CAP)

    ri = lax.broadcasted_iota(jnp.int32, (SLOTS, SLOTS), 0)
    ci = lax.broadcasted_iota(jnp.int32, (SLOTS, SLOTS), 1)
    perm[...] = jnp.where(slot_of(ri) == ci, 1.0, 0.0).astype(BF16)
    permt[...] = jnp.where(slot_of(ci) == ri, 1.0, 0.0).astype(BF16)

    for h in range(2):
        stage2_forward(h, 3)

    l_gate.wait()
    l_up.wait()
    l_down.wait()
    crow = pl.ds(pl.multiple_of(c * 64, 64), 64)
    crow_up = pl.ds(pl.multiple_of(128 + c * 64, 64), 64)
    for i in range(2):
        wall[i, 256:384, :] = jnp.zeros((128, 1024), BF16)

    def prepare(j, carry):
        mine = pl.ds(pl.multiple_of((2 * j + c) * 128, 128), 128)
        theirs = pl.ds(pl.multiple_of((2 * j + 1 - c) * 128, 128), 128)
        to = pl.ds(pl.multiple_of(j * 128, 128), 128)
        gm, gt = g2[:, mine], g2[:, theirs]
        for i in range(2):
            wall[i, crow, to] = (gate_v[i, :, mine].astype(F32) * gm).astype(BF16)
            wall[i, crow_up, to] = (up_v[i, :, mine].astype(F32) * gm).astype(BF16)
            wst[i, 0, :, to] = (gate_v[i, :, theirs].astype(F32) * gt).astype(BF16)
            wst[i, 1, :, to] = (up_v[i, :, theirs].astype(F32) * gt).astype(BF16)
            wall[i, 256:288, to] = (ert[:, mine].astype(F32) * gm).astype(BF16)
            wall[i, 288:292, to] = (grt[:, mine].astype(F32) * gm).astype(BF16)
            dn[i, crow, to] = down_v[i, :, mine]
            dst[i, :, to] = down_v[i, :, theirs]
        return carry

    lax.fori_loop(0, SZ, prepare, 0)
    w_ids = [[new_id() for _ in range(3)] for _ in range(2)]
    for i in range(2):
        rdma(w_ids[i][0], wst.at[i, 0], wall.at[i, crow, :], partner)
        rdma(w_ids[i][1], wst.at[i, 1], wall.at[i, crow_up, :], partner)
        rdma(w_ids[i][2], dst.at[i], dn.at[i, crow, :], partner)

    for h, (dev, blk) in enumerate(halves):
        for b in range(4):
            arrived(ids2[h][b, "fp"], blk(offs[b], 2, 0), (dev(0, -1), t))
            arrived(ids2[h][b, "fm"], blk(offs[b], 2, 1), (dev(0, 1), t))

    qk = mm(normed_v[...], wga[...]).astype(BF16).astype(F32)
    vo = mm(normed_v[...], wgb[...]).astype(BF16).astype(F32)

    meta_ids = {}
    for k in range(1, NEP):
        meta_ids[k] = new_id()
        pe = peer_ep(k)
        rdma(
            meta_ids[k], meta.at[pl.ds(pl.multiple_of(pe * ROWS, 8), ROWS), :],
            metar.at[pl.ds(pl.multiple_of(e * ROWS, 8), ROWS), :], (pe, t),
        )
    mine24 = pl.ds(pl.multiple_of(e * ROWS, 8), ROWS)
    metar[mine24, :] = meta[mine24, :]

    q_t = qk[:, 0:128].T * 0.125
    k_t = qk[:, 128:256].T
    v_t = vo[:, 0:128].T
    qt[...] = q_t
    l_state.wait()
    headed = []
    for h in range(2):
        rows = slice(h * 64, h * 64 + 64)
        ing = gates_v[pl.ds(2 * t + h, 1), :]
        pre = gates_v[pl.ds(32 + 2 * t + h, 1), :] + bias[2 * t + h]
        lf = jnp.minimum(pre, 0.0) - jnp.log1p(jnp.exp(-jnp.abs(pre)))
        run = lf + smax[h : h + 1, :]
        stable = jnp.maximum(run, ing)
        fresh = jnp.exp(ing - stable)
        carried = jnp.exp(run - stable)
        newmax[h : h + 1, :] = stable
        qh, kh, vh = q_t[rows, :], k_t[rows, :], v_t[rows, :]
        fk = fresh * kh
        fkt[rows, :] = fk
        nh = nrm[h]
        newnrm[h] = carried * nh + fk
        score = jnp.sum(qh * kh, axis=0, keepdims=True) * fresh
        denom = carried * jnp.sum(qh * nh, axis=0, keepdims=True) + score

        def body(j, acc, h=h, carried=carried, vh=vh):
            d0 = pl.multiple_of(h * 64 + j * 8, 8)
            q8 = qt[pl.ds(d0, 8), :]
            f8 = fkt[pl.ds(d0, 8), :]
            for r in range(8):
                m = st[h, j * 8 + r]
                acc = acc + q8[r : r + 1, :] * m
                st[h, j * 8 + r] = carried * m + f8[r : r + 1, :] * vh
            return acc

        readout = lax.fori_loop(0, 8, body, jnp.zeros((64, 128), F32))
        cell = (carried * readout + score * vh) / jnp.maximum(jnp.abs(denom), 1.0)
        headed.append(cell * lax.rsqrt(jnp.mean(cell * cell, axis=0, keepdims=True) + EPS))
    head_out = jnp.concatenate(headed, axis=0).T * hgain[...] * jax.nn.sigmoid(vo[:, 128:256])
    hg[:, zown] = head_out.astype(BF16)

    head_ids = {}
    for k in (4, 3, 5, 2, 6, 1, 7):
        head_ids[k] = new_id()
        rdma(head_ids[k], hg.at[:, zown], hg.at[:, zown], (e, 2 * zoff(k) + c))
    l_new = local(st, newmat_hbm)

    for k in range(1, NEP):
        pe = lax.rem(e - k + NEP, NEP)
        arrived(meta_ids[k], metar.at[pl.ds(pl.multiple_of(pe * ROWS, 8), ROWS), :], (pe, t))
    metap[...] = mm(perm[...], metar[...].astype(BF16))
    l_wob.wait()
    for k in range(1, SZ):
        zk = zoff(-k)
        arrived(wout_ids[k], wob.at[pl.ds(pl.multiple_of(zk * 128, 128), 128), :], (e, 2 * zk + c))
    prow = pl.ds(pl.multiple_of((1 - c) * 64, 64), 64)
    prow_up = pl.ds(pl.multiple_of(128 + (1 - c) * 64, 64), 64)
    for i in range(2):
        arrived(w_ids[i][0], wall.at[i, prow, :], partner)
        arrived(w_ids[i][1], wall.at[i, prow_up, :], partner)
        arrived(w_ids[i][2], dn.at[i, prow, :], partner)

    for k in range(1, SZ):
        zk = zoff(-k)
        arrived(head_ids[k], hg.at[:, pl.ds(pl.multiple_of(zk * 128, 128), 128)], (e, 2 * zk + c))
    att[...] = mm(hg[...], wob[...])
    att_id = new_id()
    rdma(att_id, att.at[:, pl.ds(pl.multiple_of((1 - c) * 128, 128), 128)], attr, partner)
    base = (
        resid_v[:, pl.ds(pl.multiple_of(t * 128, 128), 128)].astype(F32)
    )
    arrived(att_id, attr, partner)
    after = (base + (att[:, pl.ds(pl.multiple_of(c * 128, 128), 128)] + attr[...])).astype(BF16)
    after_v[...] = after

    dsp[...] = mm(disp[...], after)
    disp_ids = {}
    for k in range(1, NEP):
        disp_ids[k] = new_id()
        pe = peer_ep(k)
        rdma(
            disp_ids[k], dsp.at[pl.ds(pl.multiple_of(pe * ROWS, 8), ROWS), :],
            rx.at[mine24, :], (pe, t),
        )
    rx[mine24, :] = dsp[mine24, :]
    for k in range(1, NEP):
        pe = lax.rem(e - k + NEP, NEP)
        arrived(disp_ids[k], rx.at[pl.ds(pl.multiple_of(pe * ROWS, 8), ROWS), :], (pe, t))
    xg[:, zown] = mm(perm[...], rx[...].astype(BF16)).astype(BF16)

    def xblk(k, ch):
        return xg.at[pl.ds(ch * HALF, HALF), pl.ds(pl.multiple_of(zoff(k) * 128, 128), 128)]

    ag_ids = {(d, k, ch): new_id() for d in (0, 1) for k in range(1, 5) for ch in (0, 1) if k < 4 or ch == d}
    nxt = ((e, 2 * zoff(1) + c), (e, 2 * zoff(-1) + c))
    for other in (False, True):
        for d in (0, 1):
            ch = d ^ 1 if other else d
            rdma(ag_ids[d, 1, ch], xblk(0, ch), xblk(0, ch), nxt[d])
    for k in range(1, 5):
        for other in (False, True):
            for d in (0, 1):
                ch = d ^ 1 if other else d
                if (d, k, ch) not in ag_ids:
                    continue
                off = -k if d == 0 else k
                arrived(ag_ids[d, k, ch], xblk(off, ch), nxt[1 - d])
                if (d, k + 1, ch) in ag_ids:
                    rdma(ag_ids[d, k + 1, ch], xblk(off, ch), xblk(off, ch), nxt[d])

    s_ids = [new_id(), new_id()]
    lane = lax.broadcasted_iota(jnp.int32, (HALF, 384), 1)
    for i in range(2):
        rows = slice(i * HALF, (i + 1) * HALF)
        xi = xg[rows, :]
        wide = xi.astype(F32)
        square = jnp.sum(wide * wide, axis=1, keepdims=True)
        sb[rows, :] = jnp.where(lane == 383, square, mmt(xi, wall[i]))
        rdma(s_ids[i], sb.at[pl.ds(i * HALF, HALF), :], sr.at[pl.ds(i * HALF, HALF), :], partner)
    lane = lax.broadcasted_iota(jnp.int32, (HALF, 128), 1)
    logits = []
    for i in range(2):
        rows = slice(i * HALF, (i + 1) * HALF)
        arrived(s_ids[i], sr.at[pl.ds(i * HALF, HALF), :], partner)
        both = sb[rows, :] + sr[rows, :]
        f = lax.rsqrt(both[:, 383:384] * (1.0 / 2048) + EPS)
        g = both[:, 0:128] * f
        u = both[:, 128:256] * f
        units = (g / (1.0 + jnp.exp(-g)) * u).astype(BF16)
        pbuf[rows, :] = mm(units, dn[i]).astype(BF16)
        logits.append(both[:, 256:384] * f)

    rs_ids = {(d, s, ch): new_id() for d in (0, 1) for s in range(4) for ch in (0, 1) if s or ch == d}

    def pblk(zd, ch):
        return (pl.ds(ch * HALF, HALF), pl.ds(pl.multiple_of(zd * 128, 128), 128))

    def rs_send(d, s, ch):
        zd = zoff(4 - s) if d == 0 else zoff(s - 4)
        rows, cols = pblk(zd, ch)
        if (d, s - 1, ch) in rs_ids:
            arrived(rs_ids[d, s - 1, ch], rbuf.at[d, s - 1, ch], nxt[1 - d])
            sbuf[d, s, ch] = (pbuf[rows, cols].astype(F32) + rbuf[d, s - 1, ch].astype(F32)).astype(BF16)
            src = sbuf.at[d, s, ch]
        else:
            src = pbuf.at[rows, cols]
        rdma(rs_ids[d, s, ch], src, rbuf.at[d, s, ch], nxt[d])

    for d in (0, 1):
        rs_send(d, 0, d)
    for d in (0, 1):
        rs_send(d, 1, d ^ 1)
    for i in range(2):
        rows = slice(i * HALF, (i + 1) * HALF)
        exps = jnp.exp(logits[i])
        pick = metap[rows, :] > 0.5
        den = jnp.sum(jnp.where(pick, exps, 0.0), axis=1, keepdims=True)
        num = jnp.sum(jnp.where(lane == 2 * e + i, exps, 0.0), axis=1, keepdims=True)
        gden = jnp.sum(jnp.where((lane >= 32) & (lane < 36), exps, 0.0), axis=1, keepdims=True)
        gnum = jnp.sum(jnp.where(lane == 32 + e // 4, exps, 0.0), axis=1, keepdims=True)
        used = jnp.sum(jnp.where(pick, 1.0, 0.0), axis=1, keepdims=True) > 0.5
        share = jnp.where(used, num, 0.0) / jnp.where(used, den, 1.0)
        wgt[rows, :] = jnp.broadcast_to(gnum / gden * share, (HALF, 128))
    for s in (1, 2, 3):
        for d in (0, 1):
            rs_send(d, s, d)
        if s < 3:
            for d in (0, 1):
                rs_send(d, s + 1, d ^ 1)
    weighted = []
    for ch in (0, 1):
        for d in (0, 1):
            arrived(rs_ids[d, 3, ch], rbuf.at[d, 3, ch], nxt[1 - d])
        rows, cols = pblk(z, ch)
        total = pbuf[rows, cols].astype(F32) + rbuf[0, 3, ch].astype(F32) + rbuf[1, 3, ch].astype(F32)
        weighted.append((total * wgt[ch * HALF : (ch + 1) * HALF, :]).astype(BF16))
    sx[...] = mm(permt[...], jnp.concatenate(weighted, axis=0))

    ret_ids = {}
    for k in range(1, NEP):
        ret_ids[k] = new_id()
        pe = peer_ep(k)
        rdma(
            ret_ids[k], sx.at[pl.ds(pl.multiple_of(pe * ROWS, 8), ROWS), :],
            ret.at[mine24, :], (pe, t),
        )
    ret[mine24, :] = sx[mine24, :]
    for k in range(1, NEP):
        pe = lax.rem(e - k + NEP, NEP)
        arrived(ret_ids[k], ret.at[pl.ds(pl.multiple_of(pe * ROWS, 8), ROWS), :], (pe, t))
    moe = mm(dispt[...], ret[...].astype(BF16))
    mixed[...] = (after_v[...].astype(F32) + moe).astype(BF16)

    l_new.wait()
    for copy in sent:
        copy.wait_send()


def per_device(
    resid, norm1_gain, w_query, w_key, w_value, w_outgate, w_igate, w_fgate, forget_bias,
    head_gain, w_out, state_matrix, state_norm, state_max, norm2_gain, group_router,
    expert_router, expert_ids, exp_gate, exp_up, exp_down,
):
    any_ = pl.BlockSpec(memory_space=pl.ANY)
    vmem = pl.BlockSpec(memory_space=pltpu.VMEM)
    smem = pl.BlockSpec(memory_space=pltpu.SMEM)
    args = [
        (resid, any_), (norm1_gain.reshape(1, -1), vmem), (w_query, any_), (w_key, any_),
        (w_value, any_), (w_outgate, any_), (w_igate.T, vmem), (w_fgate.T, vmem),
        (forget_bias, smem), (head_gain.reshape(1, -1), vmem), (w_out, any_),
        (state_matrix.transpose(1, 2, 3, 0), any_), (state_norm.transpose(1, 2, 0), vmem),
        (state_max.T, vmem), (norm2_gain.reshape(1, -1), vmem), (group_router.T, vmem),
        (expert_router.T, vmem), (expert_ids.T, vmem), (exp_gate.transpose(0, 2, 1), any_),
        (exp_up.transpose(0, 2, 1), any_), (exp_down, any_),
    ]
    V = pltpu.VMEM
    scratch = [
        V((128, 2048), BF16), V((128, 2048), BF16), V((2048, 256), BF16), V((2048, 256), BF16),
        V((64, 128), F32), V((2, 64, 64, 128), F32), V((128, 128), F32), V((128, 128), F32),
        V((128, 1024), BF16), V((1024, 256), BF16), V((128, 256), F32), V((128, 128), F32),
        V((SLOTS, 128), BF16), V((128, SLOTS), BF16), V((SLOTS, SLOTS), BF16), V((SLOTS, SLOTS), BF16),
        V((SLOTS, 128), F32), V((SLOTS, 128), F32), V((SLOTS, 128), F32), V((SLOTS, 128), F32),
        V((SLOTS, 128), F32), V((SLOTS, 1024), BF16),
        V((2, 64, 2048), BF16), V((2, 64, 2048), BF16), V((2, 64, 2048), BF16),
        V((2, 384, 1024), BF16), V((2, 2, 64, 1024), BF16), V((2, 128, 1024), BF16), V((2, 64, 1024), BF16),
        V((SLOTS, 384), F32), V((SLOTS, 384), F32), V((SLOTS, 128), F32), V((SLOTS, 1024), BF16),
        V((2, 4, 2, HALF, 128), BF16), V((2, 4, 2, HALF, 128), BF16),
        V((SLOTS, 128), F32), V((SLOTS, 128), F32), V((128, 128), BF16),
        pltpu.SemaphoreType.DMA((NREM,)), pltpu.SemaphoreType.DMA((NREM,)), pltpu.SemaphoreType.DMA((NLOC,)),
    ]
    mixed, newmat, newnrm, newmax = pl.pallas_call(
        kernel,
        out_shape=(
            jax.ShapeDtypeStruct((128, 128), BF16),
            jax.ShapeDtypeStruct((2, 64, 64, 128), F32),
            jax.ShapeDtypeStruct((2, 64, 128), F32),
            jax.ShapeDtypeStruct((2, 128), F32),
        ),
        in_specs=[s for _, s in args],
        out_specs=(vmem, any_, vmem, vmem),
        scratch_shapes=scratch,
        compiler_params=pltpu.CompilerParams(
            collective_id=0, has_side_effects=True, vmem_limit_bytes=48 * 1024 * 1024
        ),
    )(*[a for a, _ in args])
    return mixed, newmat.transpose(3, 0, 1, 2), newnrm.transpose(2, 0, 1), newmax.T


def solution(mesh):
    in_specs = (
        P("ep", None), P(), P("ep", "tp"), P("ep", "tp"), P("ep", "tp"), P("ep", "tp"), P(), P(), P(),
        P("tp"), P("tp", None), P("ep", "tp", None, None), P("ep", "tp", None), P("ep", "tp"), P(),
        P(), P(), P("ep", None), P("ep", None, "tp"), P("ep", None, "tp"), P("ep", "tp", None),
    )
    out_specs = (P("ep", "tp"), P("ep", "tp", None, None), P("ep", "tp", None), P("ep", "tp"))
    return jax.shard_map(
        per_device, mesh=mesh, in_specs=in_specs, out_specs=out_specs, check_vma=False
    )
```

```python
import functools

import jax
import jax.numpy as jnp
from jax import lax
from jax.experimental import pallas as pl
from jax.experimental.pallas import tpu as pltpu
from jax.sharding import PartitionSpec as P

EPS = 1e-06
F32 = jnp.float32
BF16 = jnp.bfloat16
MESH = pl.DeviceIdType.MESH
SX, SY, SZ = 4, 4, 8
NEP = SX * SY
CAP = 12
ROWS = 2 * CAP
SLOTS = NEP * ROWS
HALF = SLOTS // 2
NREM = 192
NLOC = 24


def mm(a, b):
    return lax.dot_general(a, b, (((1,), (0,)), ((), ())), preferred_element_type=F32)


def mmt(a, b):
    return lax.dot_general(a, b, (((1,), (1,)), ((), ())), preferred_element_type=F32)


def by12(v):
    return (v * 43691) >> 19


def kernel(
    resid_hbm, g1_hbm, wq_hbm, wk_hbm, wv_hbm, wo_hbm, igt_hbm, fgt_hbm, bias_hbm, hgain_hbm, wout_hbm,
    st_hbm, nrm_hbm, smax_hbm, g2_hbm, grt_hbm, ert_hbm, ids_hbm, gate_hbm, up_hbm, down_hbm,
    mixed, st, newnrm, newmax,
    g1, igt, fgt, bias, hgain, nrm, smax, g2, grt, ert, ids,
    resid_v, normed_v, wga, wgb, gates_v, qt, fkt, hg, wob, att, attr,
    disp, dispt, perm, permt, meta, metar, metap, dsp, rx, xg,
    gate_v, up_v, down_v, wall, wst, dn, dst, sb, sr, wgt, pbuf, sbuf, rbuf, sx, ret, after_v,
    ssem, rsem, lsem,
):
    e = lax.axis_index("ep")
    t = lax.axis_index("tp")
    y, x = e // SX, lax.rem(e, SX)
    z, c = t // 2, lax.rem(t, 2)
    count = [0, 0]
    sent = []

    def new_id():
        count[0] += 1
        return count[0] - 1

    def rdma(k, src, dst, dev):
        copy = pltpu.make_async_remote_copy(
            src_ref=src, dst_ref=dst, send_sem=ssem.at[k], recv_sem=rsem.at[k],
            device_id=dev, device_id_type=MESH,
        )
        copy.start()
        sent.append(copy)

    def arrived(k, region, dev):
        pltpu.make_async_remote_copy(
            src_ref=region, dst_ref=region, send_sem=ssem.at[k], recv_sem=rsem.at[k],
            device_id=dev, device_id_type=MESH,
        ).wait_recv()

    def local(src, dst):
        k = count[1]
        count[1] += 1
        copy = pltpu.make_async_copy(src, dst, lsem.at[k])
        copy.start()
        return copy

    def peer_ep(k):
        return lax.rem(e + k, NEP)

    def at_xy(dx, dy):
        return lax.rem(y + dy + SY, SY) * SX + lax.rem(x + dx + SX, SX)

    def zoff(k):
        return lax.rem(z + k + SZ, SZ)

    partner = (e, 2 * z + 1 - c)

    own = pl.ds(pl.multiple_of(e * 128, 128), 128)
    l_wa = [local(wq_hbm, wga.at[own, pl.ds(0, 128)]), local(wk_hbm, wga.at[own, pl.ds(128, 128)])]
    l_wb = [local(wv_hbm, wgb.at[own, pl.ds(0, 128)]), local(wo_hbm, wgb.at[own, pl.ds(128, 128)])]
    l_resid = [local(resid_hbm, resid_v), local(g1_hbm, g1)]

    barrier = pltpu.get_barrier_semaphore()
    peers = [(peer_ep(k), t) for k in range(1, NEP)]
    peers += [(e, 2 * zoff(k) + c) for k in range(1, SZ)] + [partner]
    for p in peers:
        pl.semaphore_signal(barrier, inc=1, device_id=p, device_id_type=MESH)

    zown = pl.ds(pl.multiple_of(z * 128, 128), 128)
    l_wob = local(wout_hbm.at[:, pl.ds(pl.multiple_of(z * 256, 256), 256)], wob.at[zown, :])
    l_gates = [local(igt_hbm, igt), local(fgt_hbm, fgt), local(ids_hbm, ids)]
    l_state = [
        local(st_hbm, st), local(nrm_hbm, nrm), local(smax_hbm, smax), local(bias_hbm, bias),
        local(hgain_hbm, hgain),
    ]
    l_router = [local(g2_hbm, g2), local(grt_hbm, grt), local(ert_hbm, ert)]
    l_gate = local(gate_hbm, gate_v)
    l_up = local(up_hbm, up_v)
    l_down = local(down_hbm, down_v)

    pl.semaphore_wait(barrier, len(peers))
    for cp in l_wa + l_wb:
        cp.wait()

    halves = []
    for wg, first in ((wga, "x"), (wgb, "y")):
        def dev(a1, a2, first=first):
            return at_xy(a1, a2) if first == "x" else at_xy(a2, a1)

        def blk(a1, a2, part, wg=wg, dev=dev):
            base = dev(a1, a2) * 128
            if part is None:
                return wg.at[pl.ds(pl.multiple_of(base, 128), 128), :]
            return wg.at[pl.ds(pl.multiple_of(base + part * 64, 64), 64), :]

        halves.append((dev, blk))

    ids1 = [{k: new_id() for k in ("p", "m", "fp", "fm")} for _ in halves]
    ids2 = [{(b, k): new_id() for b in range(4) for k in ("p", "m", "fp", "fm")} for _ in halves]
    offs = (0, -1, 1, 2)

    def stage2_start(h, b):
        dev, blk = halves[h]
        rdma(ids2[h][b, "p"], blk(offs[b], 0, None), blk(offs[b], 0, None), (dev(0, 1), t))
        rdma(ids2[h][b, "m"], blk(offs[b], 0, None), blk(offs[b], 0, None), (dev(0, -1), t))

    for h, (dev, blk) in enumerate(halves):
        rdma(ids1[h]["p"], blk(0, 0, None), blk(0, 0, None), (dev(1, 0), t))
        rdma(ids1[h]["m"], blk(0, 0, None), blk(0, 0, None), (dev(-1, 0), t))
    for h in range(2):
        stage2_start(h, 0)

    wout_ids = {}
    for k in range(1, SZ):
        wout_ids[k] = new_id()
        zk = zoff(k)
        rdma(
            wout_ids[k], wout_hbm.at[:, pl.ds(pl.multiple_of(zk * 256, 256), 256)],
            wob.at[zown, :], (e, 2 * zk + c),
        )

    for cp in l_resid:
        cp.wait()
    wide = resid_v[...].astype(F32)
    factor = lax.rsqrt(jnp.mean(wide * wide, axis=1, keepdims=True) + EPS)
    normed_v[...] = (wide * factor * g1[...]).astype(BF16)

    for h, (dev, blk) in enumerate(halves):
        arrived(ids1[h]["p"], blk(-1, 0, None), (dev(-1, 0), t))
        rdma(ids1[h]["fp"], blk(-1, 0, 0), blk(-1, 0, 0), (dev(1, 0), t))
        arrived(ids1[h]["m"], blk(1, 0, None), (dev(1, 0), t))
        rdma(ids1[h]["fm"], blk(1, 0, 1), blk(1, 0, 1), (dev(-1, 0), t))
    for b in (1, 2):
        for h in range(2):
            stage2_start(h, b)

    for cp in l_gates:
        cp.wait()
    gates_v[0:32, :] = mmt(igt[...], normed_v[...])
    gates_v[32:64, :] = mmt(fgt[...], normed_v[...])

    def stage2_forward(h, b):
        dev, blk = halves[h]
        arrived(ids2[h][b, "p"], blk(offs[b], -1, None), (dev(0, -1), t))
        rdma(ids2[h][b, "fp"], blk(offs[b], -1, 0), blk(offs[b], -1, 0), (dev(0, 1), t))
        arrived(ids2[h][b, "m"], blk(offs[b], 1, None), (dev(0, 1), t))
        rdma(ids2[h][b, "fm"], blk(offs[b], 1, 1), blk(offs[b], 1, 1), (dev(0, -1), t))

    for h in range(2):
        stage2_forward(h, 0)
    for h, (dev, blk) in enumerate(halves):
        arrived(ids1[h]["fp"], blk(2, 0, 0), (dev(-1, 0), t))
        arrived(ids1[h]["fm"], blk(2, 0, 1), (dev(1, 0), t))
        stage2_start(h, 3)

    srow = lax.broadcasted_iota(jnp.int32, (SLOTS, 128), 0)
    s_exp = by12(srow)
    s_cap = srow - s_exp * CAP
    assigned = jnp.where((ids[0:1, :] == s_exp) | (ids[1:2, :] == s_exp), 1.0, 0.0)
    earlier = jnp.where(
        lax.broadcasted_iota(jnp.int32, (128, 128), 0) < lax.broadcasted_iota(jnp.int32, (128, 128), 1),
        1.0, 0.0,
    ).astype(BF16)
    rank = mm(assigned.astype(BF16), earlier)
    hot = jnp.where(jnp.abs(rank - s_cap.astype(F32)) < 0.5, assigned, 0.0)
    disp[...] = hot.astype(BF16)
    dispt[...] = hot.T.astype(BF16)
    erow = lax.broadcasted_iota(jnp.int32, (128, 128), 0)
    chosen = jnp.where((ids[0:1, :] == erow) | (ids[1:2, :] == erow), 1.0, 0.0).T.astype(BF16)
    meta[...] = mm(disp[...], chosen)

    for h in range(2):
        for b in (1, 2):
            stage2_forward(h, b)

    def slot_of(r):
        i = jnp.where(r >= HALF, 1, 0)
        q = r - i * HALF
        s = by12(q)
        return s * ROWS + i * CAP + (q - s * CAP)

    ri = lax.broadcasted_iota(jnp.int32, (SLOTS, SLOTS), 0)
    ci = lax.broadcasted_iota(jnp.int32, (SLOTS, SLOTS), 1)
    perm[...] = jnp.where(slot_of(ri) == ci, 1.0, 0.0).astype(BF16)
    permt[...] = jnp.where(slot_of(ci) == ri, 1.0, 0.0).astype(BF16)

    for h in range(2):
        stage2_forward(h, 3)

    l_gate.wait()
    l_up.wait()
    l_down.wait()
    for cp in l_router:
        cp.wait()
    crow = pl.ds(pl.multiple_of(c * 64, 64), 64)
    crow_up = pl.ds(pl.multiple_of(128 + c * 64, 64), 64)
    for i in range(2):
        wall[i, 256:384, :] = jnp.zeros((128, 1024), BF16)

    def prepare(j, carry):
        mine = pl.ds(pl.multiple_of((2 * j + c) * 128, 128), 128)
        theirs = pl.ds(pl.multiple_of((2 * j + 1 - c) * 128, 128), 128)
        to = pl.ds(pl.multiple_of(j * 128, 128), 128)
        gm, gt = g2[:, mine], g2[:, theirs]
        for i in range(2):
            wall[i, crow, to] = (gate_v[i, :, mine].astype(F32) * gm).astype(BF16)
            wall[i, crow_up, to] = (up_v[i, :, mine].astype(F32) * gm).astype(BF16)
            wst[i, 0, :, to] = (gate_v[i, :, theirs].astype(F32) * gt).astype(BF16)
            wst[i, 1, :, to] = (up_v[i, :, theirs].astype(F32) * gt).astype(BF16)
            wall[i, 256:288, to] = (ert[:, mine].astype(F32) * gm).astype(BF16)
            wall[i, 288:292, to] = (grt[:, mine].astype(F32) * gm).astype(BF16)
            dn[i, crow, to] = down_v[i, :, mine]
            dst[i, :, to] = down_v[i, :, theirs]
        return carry

    lax.fori_loop(0, SZ, prepare, 0)
    w_ids = [[new_id() for _ in range(3)] for _ in range(2)]
    for i in range(2):
        rdma(w_ids[i][0], wst.at[i, 0], wall.at[i, crow, :], partner)
        rdma(w_ids[i][1], wst.at[i, 1], wall.at[i, crow_up, :], partner)
        rdma(w_ids[i][2], dst.at[i], dn.at[i, crow, :], partner)

    for h, (dev, blk) in enumerate(halves):
        for b in range(4):
            arrived(ids2[h][b, "fp"], blk(offs[b], 2, 0), (dev(0, -1), t))
            arrived(ids2[h][b, "fm"], blk(offs[b], 2, 1), (dev(0, 1), t))

    qk = mm(normed_v[...], wga[...]).astype(BF16).astype(F32)
    vo = mm(normed_v[...], wgb[...]).astype(BF16).astype(F32)

    meta_ids = {}
    for k in range(1, NEP):
        meta_ids[k] = new_id()
        pe = peer_ep(k)
        rdma(
            meta_ids[k], meta.at[pl.ds(pl.multiple_of(pe * ROWS, 8), ROWS), :],
            metar.at[pl.ds(pl.multiple_of(e * ROWS, 8), ROWS), :], (pe, t),
        )
    mine24 = pl.ds(pl.multiple_of(e * ROWS, 8), ROWS)
    metar[mine24, :] = meta[mine24, :]

    q_t = qk[:, 0:128].T * 0.125
    k_t = qk[:, 128:256].T
    v_t = vo[:, 0:128].T
    qt[...] = q_t
    for cp in l_state:
        cp.wait()
    headed = []
    for h in range(2):
        rows = slice(h * 64, h * 64 + 64)
        ing = gates_v[pl.ds(2 * t + h, 1), :]
        pre = gates_v[pl.ds(32 + 2 * t + h, 1), :] + bias[2 * t + h]
        lf = jnp.minimum(pre, 0.0) - jnp.log1p(jnp.exp(-jnp.abs(pre)))
        run = lf + smax[h : h + 1, :]
        stable = jnp.maximum(run, ing)
        fresh = jnp.exp(ing - stable)
        carried = jnp.exp(run - stable)
        newmax[h : h + 1, :] = stable
        qh, kh, vh = q_t[rows, :], k_t[rows, :], v_t[rows, :]
        fk = fresh * kh
        fkt[rows, :] = fk
        nh = nrm[h]
        newnrm[h] = carried * nh + fk
        score = jnp.sum(qh * kh, axis=0, keepdims=True) * fresh
        denom = carried * jnp.sum(qh * nh, axis=0, keepdims=True) + score

        def body(j, acc, h=h, carried=carried, vh=vh):
            d0 = pl.multiple_of(h * 64 + j * 8, 8)
            q8 = qt[pl.ds(d0, 8), :]
            f8 = fkt[pl.ds(d0, 8), :]
            for r in range(8):
                m = st[h, j * 8 + r]
                acc = acc + q8[r : r + 1, :] * m
                st[h, j * 8 + r] = carried * m + f8[r : r + 1, :] * vh
            return acc

        readout = lax.fori_loop(0, 8, body, jnp.zeros((64, 128), F32))
        cell = (carried * readout + score * vh) / jnp.maximum(jnp.abs(denom), 1.0)
        headed.append(cell * lax.rsqrt(jnp.mean(cell * cell, axis=0, keepdims=True) + EPS))
    head_out = jnp.concatenate(headed, axis=0).T * hgain[...] * jax.nn.sigmoid(vo[:, 128:256])
    hg[:, zown] = head_out.astype(BF16)

    head_ids = {}
    for k in (4, 3, 5, 2, 6, 1, 7):
        head_ids[k] = new_id()
        rdma(head_ids[k], hg.at[:, zown], hg.at[:, zown], (e, 2 * zoff(k) + c))

    for k in range(1, NEP):
        pe = lax.rem(e - k + NEP, NEP)
        arrived(meta_ids[k], metar.at[pl.ds(pl.multiple_of(pe * ROWS, 8), ROWS), :], (pe, t))
    metap[...] = mm(perm[...], metar[...].astype(BF16))
    l_wob.wait()
    for k in range(1, SZ):
        zk = zoff(-k)
        arrived(wout_ids[k], wob.at[pl.ds(pl.multiple_of(zk * 128, 128), 128), :], (e, 2 * zk + c))
    prow = pl.ds(pl.multiple_of((1 - c) * 64, 64), 64)
    prow_up = pl.ds(pl.multiple_of(128 + (1 - c) * 64, 64), 64)
    for i in range(2):
        arrived(w_ids[i][0], wall.at[i, prow, :], partner)
        arrived(w_ids[i][1], wall.at[i, prow_up, :], partner)
        arrived(w_ids[i][2], dn.at[i, prow, :], partner)

    for k in range(1, SZ):
        zk = zoff(-k)
        arrived(head_ids[k], hg.at[:, pl.ds(pl.multiple_of(zk * 128, 128), 128)], (e, 2 * zk + c))
    att[...] = mm(hg[...], wob[...])
    att_id = new_id()
    rdma(att_id, att.at[:, pl.ds(pl.multiple_of((1 - c) * 128, 128), 128)], attr, partner)
    base = (
        resid_v[:, pl.ds(pl.multiple_of(t * 128, 128), 128)].astype(F32)
    )
    arrived(att_id, attr, partner)
    after = (base + (att[:, pl.ds(pl.multiple_of(c * 128, 128), 128)] + attr[...])).astype(BF16)
    after_v[...] = after

    dsp[...] = mm(disp[...], after)
    disp_ids = {}
    for k in range(1, NEP):
        disp_ids[k] = new_id()
        pe = peer_ep(k)
        rdma(
            disp_ids[k], dsp.at[pl.ds(pl.multiple_of(pe * ROWS, 8), ROWS), :],
            rx.at[mine24, :], (pe, t),
        )
    rx[mine24, :] = dsp[mine24, :]
    for k in range(1, NEP):
        pe = lax.rem(e - k + NEP, NEP)
        arrived(disp_ids[k], rx.at[pl.ds(pl.multiple_of(pe * ROWS, 8), ROWS), :], (pe, t))
    xg[:, zown] = mm(perm[...], rx[...].astype(BF16)).astype(BF16)

    def xblk(k, ch):
        return xg.at[pl.ds(ch * HALF, HALF), pl.ds(pl.multiple_of(zoff(k) * 128, 128), 128)]

    ag_ids = {(d, k, ch): new_id() for d in (0, 1) for k in range(1, 5) for ch in (0, 1) if k < 4 or ch == d}
    nxt = ((e, 2 * zoff(1) + c), (e, 2 * zoff(-1) + c))
    for other in (False, True):
        for d in (0, 1):
            ch = d ^ 1 if other else d
            rdma(ag_ids[d, 1, ch], xblk(0, ch), xblk(0, ch), nxt[d])
    for k in range(1, 5):
        for other in (False, True):
            for d in (0, 1):
                ch = d ^ 1 if other else d
                if (d, k, ch) not in ag_ids:
                    continue
                off = -k if d == 0 else k
                arrived(ag_ids[d, k, ch], xblk(off, ch), nxt[1 - d])
                if (d, k + 1, ch) in ag_ids:
                    rdma(ag_ids[d, k + 1, ch], xblk(off, ch), xblk(off, ch), nxt[d])

    s_ids = [new_id(), new_id()]
    lane = lax.broadcasted_iota(jnp.int32, (HALF, 384), 1)
    for i in range(2):
        rows = slice(i * HALF, (i + 1) * HALF)
        xi = xg[rows, :]
        wide = xi.astype(F32)
        square = jnp.sum(wide * wide, axis=1, keepdims=True)
        sb[rows, :] = jnp.where(lane == 383, square, mmt(xi, wall[i]))
        rdma(s_ids[i], sb.at[pl.ds(i * HALF, HALF), :], sr.at[pl.ds(i * HALF, HALF), :], partner)
    lane = lax.broadcasted_iota(jnp.int32, (HALF, 128), 1)
    logits = []
    for i in range(2):
        rows = slice(i * HALF, (i + 1) * HALF)
        arrived(s_ids[i], sr.at[pl.ds(i * HALF, HALF), :], partner)
        both = sb[rows, :] + sr[rows, :]
        f = lax.rsqrt(both[:, 383:384] * (1.0 / 2048) + EPS)
        g = both[:, 0:128] * f
        u = both[:, 128:256] * f
        units = (g / (1.0 + jnp.exp(-g)) * u).astype(BF16)
        pbuf[rows, :] = mm(units, dn[i]).astype(BF16)
        logits.append(both[:, 256:384] * f)

    rs_ids = {(d, s, ch): new_id() for d in (0, 1) for s in range(4) for ch in (0, 1) if s or ch == d}

    def pblk(zd, ch):
        return (pl.ds(ch * HALF, HALF), pl.ds(pl.multiple_of(zd * 128, 128), 128))

    def rs_send(d, s, ch):
        zd = zoff(4 - s) if d == 0 else zoff(s - 4)
        rows, cols = pblk(zd, ch)
        if (d, s - 1, ch) in rs_ids:
            arrived(rs_ids[d, s - 1, ch], rbuf.at[d, s - 1, ch], nxt[1 - d])
            sbuf[d, s, ch] = (pbuf[rows, cols].astype(F32) + rbuf[d, s - 1, ch].astype(F32)).astype(BF16)
            src = sbuf.at[d, s, ch]
        else:
            src = pbuf.at[rows, cols]
        rdma(rs_ids[d, s, ch], src, rbuf.at[d, s, ch], nxt[d])

    for d in (0, 1):
        rs_send(d, 0, d)
    for d in (0, 1):
        rs_send(d, 1, d ^ 1)
    for i in range(2):
        rows = slice(i * HALF, (i + 1) * HALF)
        exps = jnp.exp(logits[i])
        pick = metap[rows, :] > 0.5
        den = jnp.sum(jnp.where(pick, exps, 0.0), axis=1, keepdims=True)
        num = jnp.sum(jnp.where(lane == 2 * e + i, exps, 0.0), axis=1, keepdims=True)
        gden = jnp.sum(jnp.where((lane >= 32) & (lane < 36), exps, 0.0), axis=1, keepdims=True)
        gnum = jnp.sum(jnp.where(lane == 32 + e // 4, exps, 0.0), axis=1, keepdims=True)
        used = jnp.sum(jnp.where(pick, 1.0, 0.0), axis=1, keepdims=True) > 0.5
        share = jnp.where(used, num, 0.0) / jnp.where(used, den, 1.0)
        wgt[rows, :] = jnp.broadcast_to(gnum / gden * share, (HALF, 128))
    for s in (1, 2, 3):
        for d in (0, 1):
            rs_send(d, s, d)
        if s < 3:
            for d in (0, 1):
                rs_send(d, s + 1, d ^ 1)
    weighted = []
    for ch in (0, 1):
        for d in (0, 1):
            arrived(rs_ids[d, 3, ch], rbuf.at[d, 3, ch], nxt[1 - d])
        rows, cols = pblk(z, ch)
        total = pbuf[rows, cols].astype(F32) + rbuf[0, 3, ch].astype(F32) + rbuf[1, 3, ch].astype(F32)
        weighted.append((total * wgt[ch * HALF : (ch + 1) * HALF, :]).astype(BF16))
    sx[...] = mm(permt[...], jnp.concatenate(weighted, axis=0))

    ret_ids = {}
    for k in range(1, NEP):
        ret_ids[k] = new_id()
        pe = peer_ep(k)
        rdma(
            ret_ids[k], sx.at[pl.ds(pl.multiple_of(pe * ROWS, 8), ROWS), :],
            ret.at[mine24, :], (pe, t),
        )
    ret[mine24, :] = sx[mine24, :]
    for k in range(1, NEP):
        pe = lax.rem(e - k + NEP, NEP)
        arrived(ret_ids[k], ret.at[pl.ds(pl.multiple_of(pe * ROWS, 8), ROWS), :], (pe, t))
    moe = mm(dispt[...], ret[...].astype(BF16))
    mixed[...] = (after_v[...].astype(F32) + moe).astype(BF16)

    for copy in sent:
        copy.wait_send()


def write_out(*refs):
    sems = refs[8]
    copies = [pltpu.make_async_copy(refs[k], refs[4 + k], sems.at[k]) for k in range(4)]
    for cp in copies:
        cp.start()
    for cp in copies:
        cp.wait()


def per_device(
    resid, norm1_gain, w_query, w_key, w_value, w_outgate, w_igate, w_fgate, forget_bias,
    head_gain, w_out, state_matrix, state_norm, state_max, norm2_gain, group_router,
    expert_router, expert_ids, exp_gate, exp_up, exp_down,
):
    hbm = pl.BlockSpec(memory_space=pltpu.HBM)
    vmem = pl.BlockSpec(memory_space=pltpu.VMEM)
    args = [
        resid, norm1_gain.reshape(1, -1), w_query, w_key, w_value, w_outgate, w_igate.T, w_fgate.T,
        forget_bias, head_gain.reshape(1, -1), w_out, state_matrix.transpose(1, 2, 3, 0),
        state_norm.transpose(1, 2, 0), state_max.T, norm2_gain.reshape(1, -1), group_router.T,
        expert_router.T, expert_ids.T, exp_gate.transpose(0, 2, 1), exp_up.transpose(0, 2, 1), exp_down,
    ]
    V = pltpu.VMEM
    scratch = [
        V((1, 2048), F32), V((32, 2048), BF16), V((32, 2048), BF16), pltpu.SMEM((32,), F32), V((1, 128), F32),
        V((2, 64, 128), F32), V((2, 128), F32), V((1, 2048), F32), V((4, 2048), BF16), V((32, 2048), BF16),
        V((2, 128), jnp.int32),
        V((128, 2048), BF16), V((128, 2048), BF16), V((2048, 256), BF16), V((2048, 256), BF16),
        V((64, 128), F32), V((128, 128), F32), V((128, 128), F32),
        V((128, 1024), BF16), V((1024, 256), BF16), V((128, 256), F32), V((128, 128), F32),
        V((SLOTS, 128), BF16), V((128, SLOTS), BF16), V((SLOTS, SLOTS), BF16), V((SLOTS, SLOTS), BF16),
        V((SLOTS, 128), F32), V((SLOTS, 128), F32), V((SLOTS, 128), F32), V((SLOTS, 128), F32),
        V((SLOTS, 128), F32), V((SLOTS, 1024), BF16),
        V((2, 64, 2048), BF16), V((2, 64, 2048), BF16), V((2, 64, 2048), BF16),
        V((2, 384, 1024), BF16), V((2, 2, 64, 1024), BF16), V((2, 128, 1024), BF16), V((2, 64, 1024), BF16),
        V((SLOTS, 384), F32), V((SLOTS, 384), F32), V((SLOTS, 128), F32), V((SLOTS, 1024), BF16),
        V((2, 4, 2, HALF, 128), BF16), V((2, 4, 2, HALF, 128), BF16),
        V((SLOTS, 128), F32), V((SLOTS, 128), F32), V((128, 128), BF16),
        pltpu.SemaphoreType.DMA((NREM,)), pltpu.SemaphoreType.DMA((NREM,)), pltpu.SemaphoreType.DMA((NLOC,)),
    ]
    shapes = (
        jax.ShapeDtypeStruct((128, 128), BF16),
        jax.ShapeDtypeStruct((2, 64, 64, 128), F32),
        jax.ShapeDtypeStruct((2, 64, 128), F32),
        jax.ShapeDtypeStruct((2, 128), F32),
    )
    results = pl.pallas_call(
        kernel,
        out_shape=shapes,
        in_specs=[hbm] * len(args),
        out_specs=(vmem,) * 4,
        scratch_shapes=scratch,
        compiler_params=pltpu.CompilerParams(
            collective_id=0, has_side_effects=True, vmem_limit_bytes=40 * 1024 * 1024
        ),
    )(*[pltpu.with_memory_space_constraint(a, pltpu.HBM) for a in args])
    mixed, newmat, newnrm, newmax = pl.pallas_call(
        write_out,
        out_shape=shapes,
        in_specs=[vmem] * 4,
        out_specs=(hbm,) * 4,
        scratch_shapes=[pltpu.SemaphoreType.DMA((4,))],
        compiler_params=pltpu.CompilerParams(vmem_limit_bytes=16 * 1024 * 1024),
    )(*results)
    return mixed, newmat.transpose(3, 0, 1, 2), newnrm.transpose(2, 0, 1), newmax.T


def solution(mesh):
    in_specs = (
        P("ep", None), P(), P("ep", "tp"), P("ep", "tp"), P("ep", "tp"), P("ep", "tp"), P(), P(), P(),
        P("tp"), P("tp", None), P("ep", "tp", None, None), P("ep", "tp", None), P("ep", "tp"), P(),
        P(), P(), P("ep", None), P("ep", None, "tp"), P("ep", None, "tp"), P("ep", "tp", None),
    )
    out_specs = (P("ep", "tp"), P("ep", "tp", None, None), P("ep", "tp", None), P("ep", "tp"))
    return jax.shard_map(
        per_device, mesh=mesh, in_specs=in_specs, out_specs=out_specs, check_vma=False
    )
```
